32 devices in a mesh: ep: 16 (over z, y, x), tp: 2 (over core).
Axes of the slice: x: 2, y: 2, z: 4, core: 2. Of those that a mesh axis runs over, the one named last changes fastest.
Arguments:
- tokens: bfloat16 [384, 4096], P('ep'), may hold values from -6 to 6
- in_gain: float32 [4096], replicated, may hold values from 0.1 to 1.9
- routes: int32 [384, 6], P('ep'), may hold values from 0 to 15, all different within a row; in each aligned block of 24 rows (0 to 23, 24 to 47, ...) at most 10 rows name the same one
- gates: float32 [384, 6], P('ep'), may hold values from 0.25 to 1.5
- expert_gate: bfloat16 [16, 512, 4096], P('ep', 'tp'), may hold values from -0.09375 to 0.09375
- expert_up: bfloat16 [16, 512, 4096], P('ep', 'tp'), may hold values from -0.09375 to 0.09375
- expert_down: bfloat16 [16, 512, 4096], P('ep', None, 'tp'), may hold values from -0.25 to 0.25
- shared_gate: bfloat16 [512, 4096], P('tp'), may hold values from -0.09375 to 0.09375
- shared_up: bfloat16 [512, 4096], P('tp'), may hold values from -0.09375 to 0.09375
- shared_down: bfloat16 [512, 4096], P(None, 'tp')
- out_gain: float32 [4096], P('tp'), may hold values from 0.1 to 1.9
Outputs:
- mixed: bfloat16 [384, 4096], P('ep', 'tp')
The draws below stay inside these ranges and needn't reach their ends.
Inputs may be any that keep to these rules, and one draw needn't show every extreme that they name: `routes`: each row names 6 different experts; among the 24 rows of one index of ep no expert is named more than 10 times, and on some index of ep some expert is named exactly 10 times.
All inputs are finite; a program needn't handle non-finite values.
Results may differ from the reference program's by a relative error of at most 0.0075.
Values may be sent and summed in bfloat16 or wider, within the bound.
A program may use at most 64 MiB of HBM per device.

```python
import math
import jax
import jax.numpy as jnp
import numpy as np
from jax import lax

D = 4096
FF = 512
SF = 512
TOPK = 6
TOK_DEV = 24
EXPERTS = 16
TOKENS = 384
CAP = 10


def draw_shared_down(key, part):
    block_width = min(128, D)
    blocks = D // block_width
    first, second = jax.random.split(jax.random.fold_in(key, 11))
    scales = jnp.exp(jax.random.uniform(first, (blocks,), jnp.float32, -1.2, 1.2))
    column_scale = jnp.repeat(scales, block_width)
    values = jax.random.normal(second, (SF, D), jnp.float32) * SF ** (-0.5)
    return (values * column_scale[None, :]).astype(jnp.bfloat16)


def steps_of(stream_key, shape, pieces, smallest, high):
    def one(axis_at, blocks):
        draws = jax.random.uniform(jax.random.fold_in(jax.random.fold_in(stream_key, 6), axis_at), (blocks,), jnp.float32, smallest / len(pieces), high / len(pieces))
        return jnp.repeat(jnp.exp(draws), shape[axis_at] // blocks).reshape((-1,) + (1,) * (len(shape) - axis_at - 1))

    factor_of = one(*pieces[0])
    for cut in pieces[1:]:
        factor_of = factor_of * one(*cut)
    return factor_of


def deal_out(rng, own, number, rows, number_of, top, limit, skew):
    ranking = jax.random.permutation(rng, number_of)
    packed, common = load_shares(number_of, rows * top, limit, skew, True), load_shares(number_of, rows * top, limit, skew, False)
    places = jnp.arange(number_of)

    def named(tallies, offset_by):
        used = int((tallies > 0).sum())
        fixed = max(1, used // 4)
        shifted = fixed + (places - fixed + offset_by * (used - fixed)) % max(1, number_of - fixed)
        return jnp.zeros((number_of,), jnp.int32).at[ranking[jnp.where(places < fixed, places, shifted)]].set(jnp.asarray(tallies, jnp.int32))

    tallies = jnp.where(number % 4 == 0, named(packed, number // 4), named(common, number - number // 4 - 1))
    mixed = jax.random.permutation(jax.random.fold_in(own, 3), number_of)
    source_of, taker = mixed[0:number_of // 2 * 2:2], mixed[1:number_of // 2 * 2:2]
    slack = jnp.minimum(tallies[source_of] - 1, limit - tallies[taker]) // 2
    slack = jnp.where((source_of == ranking[0]) | (taker == ranking[0]) | (tallies[taker] == 0), 0, jnp.maximum(slack, 0))
    shifted = jax.random.randint(jax.random.fold_in(own, 4), (number_of // 2,), 0, 1 << 20) % (slack + 1)
    tallies = tallies.at[source_of].add(-shifted).at[taker].add(shifted)
    members = jnp.searchsorted(jnp.cumsum(tallies), jnp.arange(rows * top), side="right").astype(jnp.int32)
    listing = members.reshape(top, rows).T
    listing = listing[jax.random.permutation(jax.random.fold_in(own, 1), rows)]
    offset_by = jax.random.randint(jax.random.fold_in(own, 2), (rows, 1), 0, top)
    return jnp.take_along_axis(listing, (jnp.arange(top)[None, :] + offset_by) % top, axis=1)


def load_shares(number_of, total, reach, lean, full):
    weights = [(1 << 20) // math.isqrt(grade ** lean) + 1 for grade in range(1, number_of + 1)]
    largest = reach if full else min(reach, max(-(-total // number_of), total * weights[0] // sum(weights)))
    least = 1 if total - largest >= number_of - 1 else 0
    given, surplus = [largest] + [least] * (number_of - 1), total - largest - least * (number_of - 1)
    while surplus > 0:
        free = [i for i in range(1, number_of) if given[i] < largest] or [i for i in range(1, number_of) if given[i] < reach]
        mass, remaining = sum([weights[i] for i in free]), surplus
        for i in free:
            extra = min(reach - given[i], max(1, remaining * weights[i] // mass), surplus)
            given[i] = given[i] + extra
            surplus = surplus - extra
    return np.array(given)


def scatter_about(own_key, dims, spread, reach, shards=(), held_as=jnp.bfloat16):
    factor_of = steps_of(own_key, dims, shards, -0.22, 0.18) if shards else 1.0
    array = jax.random.normal(own_key, dims, jnp.float32) * spread * factor_of
    return jnp.minimum(jnp.maximum(array, -reach), reach).astype(held_as)


def setup_inputs(seed: int = 0) -> dict:
    streams_of = jax.random.split(jax.random.key(seed), 12)
    tokens = scatter_about(streams_of[0], (TOKENS, D), 1.0, 6.0, ((0, 16),))
    in_gain = jnp.clip(1.0 + 0.18 * jax.random.normal(streams_of[1], (D,), jnp.float32), 0.1, 1.9)
    routes_keys = jax.random.split(jax.random.fold_in(streams_of[2], 1), TOKENS // TOK_DEV)
    routes_turns = jax.random.permutation(jax.random.fold_in(streams_of[2], 3), TOKENS // TOK_DEV)
    routes = jax.vmap(lambda own, number: deal_out(jax.random.fold_in(streams_of[2], 2), own, number, TOK_DEV, EXPERTS, TOPK, CAP, 2))(routes_keys, routes_turns).reshape((TOKENS, TOPK))
    gates = jnp.clip(0.25 + 1.25 * jax.random.uniform(streams_of[3], (TOKENS, TOPK), jnp.float32) ** steps_of(streams_of[3], (TOKENS, TOPK), ((0, 16),), -0.2, 0.2), 0.25, 1.5)
    expert_gate = scatter_about(streams_of[4], (EXPERTS, FF, D), D ** -0.5, 0.09375, ((0, 16), (1, 2)))
    expert_up = scatter_about(streams_of[5], (EXPERTS, FF, D), D ** -0.5, 0.09375, ((0, 16), (1, 2)))
    expert_down = scatter_about(streams_of[6], (EXPERTS, FF, D), FF ** -0.5, 0.25, ((0, 16), (2, 2)))
    shared_gate = scatter_about(streams_of[7], (SF, D), D ** -0.5, 0.09375, ((0, 2),))
    shared_up = scatter_about(streams_of[8], (SF, D), D ** -0.5, 0.09375, ((0, 2),))
    shared_down = draw_shared_down(jax.random.fold_in(streams_of[11], 71), 0)
    out_gain = jnp.clip(1.0 + 0.18 * jax.random.normal(streams_of[10], (D,), jnp.float32), 0.1, 1.9)
    return dict(tokens=tokens, in_gain=in_gain, routes=routes, gates=gates, expert_gate=expert_gate, expert_up=expert_up, expert_down=expert_down, shared_gate=shared_gate, shared_up=shared_up, shared_down=shared_down, out_gain=out_gain)


EPS = 1e-06

def norm_rows(values, gain):
    return values * lax.rsqrt(lax.optimization_barrier(jnp.mean(values * values, axis=1, keepdims=True)) + EPS) * gain

def project(rows, weight):
    return lax.dot_general(rows, weight, (((1,), (1,)), ((), ())), preferred_element_type=jnp.float32)

def reference(tokens, in_gain, routes, gates, expert_gate, expert_up, expert_down, shared_gate, shared_up, shared_down, out_gain):
    normed = norm_rows(tokens.astype(jnp.float32), in_gain.astype(jnp.float32)).astype(jnp.bfloat16)
    shared_hidden = (jax.nn.silu(project(normed, shared_gate)) * project(normed, shared_up)).astype(jnp.bfloat16)
    shared_out = jnp.dot(shared_hidden, shared_down, preferred_element_type=jnp.float32)

    def expert_step(running, inputs):
        w_gate, w_up, w_down, index = inputs
        hidden = (jax.nn.silu(project(normed, w_gate)) * project(normed, w_up)).astype(jnp.bfloat16)
        outputs = jnp.dot(hidden, w_down, preferred_element_type=jnp.float32).astype(jnp.bfloat16)
        weight = lax.optimization_barrier(jnp.sum(jnp.where(routes == index, gates, 0.0), axis=1))
        return (running + weight[:, None] * outputs.astype(jnp.float32), None)
    start = jnp.zeros((tokens.shape[0], tokens.shape[1]), jnp.float32)
    routed, _ = lax.scan(expert_step, start, (expert_gate, expert_up, expert_down, jnp.arange(EXPERTS, dtype=jnp.int32)))
    combined = routed + shared_out
    return norm_rows(combined, out_gain.astype(jnp.float32)).astype(jnp.bfloat16)
```

```python
import functools

import jax
import jax.numpy as jnp
from jax import lax
from jax.experimental import pallas as pl
from jax.experimental.pallas import tpu as pltpu
from jax.sharding import PartitionSpec as P

EPS = 1e-06
MESH = pl.DeviceIdType.MESH
F32 = jnp.float32
BF16 = jnp.bfloat16
OWN, FAR = 0, 1
SHARED, HIDDEN, SQUARES = 0, 1, 3


def dot_nt(a, b):
    return lax.dot_general(a, b, (((1,), (1,)), ((), ())), preferred_element_type=F32)


def dot_nn(a, b):
    return jnp.dot(a, b, preferred_element_type=F32)


def silu_mul(g, u):
    return g / (1.0 + jnp.exp(-g)) * u


def kernel(
    experts, fulls, rest, chunks,
    tok_h, ing_h, routes_h, gates_h, eg, eu, ed, sg, su, sd, outg_h,
    o,
    tok, ing, routes, gates, outg,
    vg, vu, vd, vsg, vsu, vsd,
    nrm, far_x, info, far_info, send, recv, acc_g, acc_u, hbuf, shbuf, outb, ret, psend, precv, comb, sq,
    isem, wsem, lsem, csend, crecv, dsend, drecv, fsend, frecv, rsend, rrecv, psent, pgot, xsend, xrecv,
):
    me = lax.axis_index("ep")
    tp = lax.axis_index("tp")
    rows, width = tok.shape
    group = lax.axis_size("tp")
    half = width // group
    mates = experts // 2
    side = me // mates
    spot = lax.rem(me, mates)
    pal = lax.rem(me + mates, experts)
    slots = mates * 8
    span = half // chunks
    folds = 8 // rest if rest else 1
    kc = span // folds if rest else min(512, span)
    blocks = fulls + (1 if rest else 0)

    def mate(k):
        return side * mates + k

    def turn(k):
        return lax.rem(spot + k, mates)

    barrier = pltpu.get_barrier_semaphore()

    @pl.loop(1, mates)
    def _(k):
        pl.semaphore_signal(
            barrier, inc=1, device_id=(mate(turn(k)), tp), device_id_type=MESH
        )

    pl.semaphore_signal(barrier, inc=1, device_id=(pal, tp), device_id_type=MESH)
    for q in range(1, group):
        pl.semaphore_signal(
            barrier, inc=1, device_id=(me, lax.rem(tp + q, group)), device_id_type=MESH
        )

    smalls = [
        pltpu.make_async_copy(src, dst, isem.at[i])
        for i, (src, dst) in enumerate(
            ((tok_h, tok), (ing_h, ing), (routes_h, routes), (gates_h, gates), (outg_h, outg))
        )
    ]
    loads = [
        pltpu.make_async_copy(src, dst, wsem.at[i])
        for i, (src, dst) in enumerate(
            ((sg, vsg), (su, vsu), (eg.at[0], vg), (eu.at[0], vu), (ed.at[0], vd), (sd, vsd))
        )
    ]
    for load in smalls + loads:
        load.start()

    smalls[2].wait()
    smalls[3].wait()
    expert_ids = lax.broadcasted_iota(jnp.int32, (mates, rows), 0)

    def weights_for(first):
        weight_t = jnp.zeros((mates, rows), F32)
        for k in range(routes.shape[0]):
            hit = routes[k : k + 1, :] == expert_ids + first
            weight_t = jnp.where(hit, gates[k : k + 1, :], weight_t)
        return weight_t

    own_weight = weights_for(side * mates)
    info[...] = jnp.zeros_like(info)
    info[:, :rows] = weights_for((1 - side) * mates)

    smalls[0].wait()
    smalls[1].wait()
    x = tok[...].astype(F32)
    scale = lax.rsqrt(jnp.mean(x * x, axis=1, keepdims=True) + EPS)

    def normalize(part):
        cols = pl.ds(pl.multiple_of(part * half, half), half)
        nrm[part] = (tok[:, cols].astype(F32) * scale * ing[:, cols]).astype(BF16)

    normalize(tp)

    token_r = lax.broadcasted_iota(jnp.int32, (rows, rows), 0)
    token_c = lax.broadcasted_iota(jnp.int32, (rows, rows), 1)
    earlier = (token_r < token_c).astype(F32).astype(BF16)
    eye = (token_r == token_c).astype(F32).astype(BF16)
    spread_t = (
        lax.broadcasted_iota(jnp.int32, (slots, mates), 0) // 8
        == lax.broadcasted_iota(jnp.int32, (slots, mates), 1)
    ).astype(F32).astype(BF16)
    spread = (
        lax.broadcasted_iota(jnp.int32, (mates, slots), 1) // 8
        == lax.broadcasted_iota(jnp.int32, (mates, slots), 0)
    ).astype(F32).astype(BF16)

    def places(slot):
        row = slot % 8
        listed = [((8 * i + row).astype(F32), None) for i in range(fulls)]
        if rest:
            listed.append(((8 * fulls + row % rest).astype(F32), row // rest))
        return listed

    def ranked(weight_t):
        chosen_t = jnp.where(weight_t > 0.0, 1.0, 0.0).astype(BF16)
        return chosen_t, dot_nn(chosen_t, earlier).astype(BF16)

    def pickers(weight_t):
        chosen_t, rank_t = ranked(weight_t)
        named = dot_nn(spread_t, chosen_t) > 0.5
        ranks = dot_nn(spread_t, rank_t)
        made = []
        for place, piece in places(lax.broadcasted_iota(jnp.int32, (slots, rows), 0)):
            here = jnp.where(named & (ranks == place), 1.0, 0.0)
            if piece is None:
                made.append(here.astype(BF16))
            else:
                made.append([jnp.where(piece == c, here, 0.0).astype(BF16) for c in range(folds)])
        return made

    def mixers(weight_t):
        chosen_t, rank_t = ranked(weight_t)
        coarse_t = weight_t.astype(BF16)
        fine_t = (weight_t - coarse_t.astype(F32)).astype(BF16)
        named, ranks, coarse, fine = [
            dot_nn(dot_nt(eye, t).astype(BF16), spread)
            for t in (chosen_t, rank_t, coarse_t, fine_t)
        ]
        made = []
        for place, piece in places(lax.broadcasted_iota(jnp.int32, (rows, slots), 1)):
            made.append(((named > 0.5) & (ranks == place), piece))
        return made, coarse, fine

    def pick(picker, source, s, ch):
        for i in range(fulls):
            for c in range(span // kc):
                send[s, ch, :, i * span + c * kc : i * span + (c + 1) * kc] = dot_nn(
                    picker[i], source(ch * span + c * kc)
                ).astype(BF16)
        if rest:
            send[s, ch, :, fulls * span :] = sum(
                dot_nn(picker[fulls][c], source(ch * span + c * kc)) for c in range(folds)
            ).astype(BF16)

    own_picker = pickers(own_weight)
    for ch in range(chunks):
        pick(own_picker, lambda at: nrm[tp, :, at : at + kc], OWN, ch)

    def block(index):
        return pl.ds(pl.multiple_of(index * 8, 8), 8)

    def cross_info():
        return pltpu.make_async_remote_copy(
            src_ref=info, dst_ref=far_info, send_sem=csend.at[chunks], recv_sem=crecv.at[chunks],
            device_id=(pal, tp), device_id_type=MESH,
        )

    def cross(ch):
        cols = pl.ds(ch * span, span)
        return pltpu.make_async_remote_copy(
            src_ref=nrm.at[tp, :, cols], dst_ref=far_x.at[:, cols],
            send_sem=csend.at[ch], recv_sem=crecv.at[ch],
            device_id=(pal, tp), device_id_type=MESH,
        )

    def cross_back(ch):
        cols = pl.ds(ch * span, span)
        return pltpu.make_async_remote_copy(
            src_ref=psend.at[:, cols], dst_ref=precv.at[:, cols],
            send_sem=psent.at[ch], recv_sem=pgot.at[ch],
            device_id=(pal, tp), device_id_type=MESH,
        )

    def dispatch(s, ch, dest, source):
        return pltpu.make_async_remote_copy(
            src_ref=send.at[s, ch, block(dest)],
            dst_ref=recv.at[tp, s, ch, block(source)],
            send_sem=dsend.at[s, ch, dest],
            recv_sem=drecv.at[s, ch, source],
            device_id=(mate(dest), tp),
            device_id_type=MESH,
        )

    def stay(s, ch):
        return pltpu.make_async_copy(
            send.at[s, ch, block(spot)], recv.at[tp, s, ch, block(spot)], lsem.at[0, s, ch]
        )

    def forward(part, s, ch, source, q):
        return pltpu.make_async_remote_copy(
            src_ref=recv.at[part, s, ch, block(source)],
            dst_ref=recv.at[part, s, ch, block(source)],
            send_sem=fsend.at[q, s, ch, source],
            recv_sem=frecv.at[part, s, ch, source],
            device_id=(me, lax.rem(tp + q, group)),
            device_id_type=MESH,
        )

    def give_back(s, ch, dest, source):
        return pltpu.make_async_remote_copy(
            src_ref=outb.at[s, ch, block(dest)],
            dst_ref=ret.at[s, ch, block(source)],
            send_sem=rsend.at[s, ch, dest],
            recv_sem=rrecv.at[s, ch, source],
            device_id=(mate(dest), tp),
            device_id_type=MESH,
        )

    def stay_back(s, ch):
        return pltpu.make_async_copy(
            outb.at[s, ch, block(spot)], ret.at[s, ch, block(spot)], lsem.at[1, s, ch]
        )

    def swap(view, i, part, q):
        return pltpu.make_async_remote_copy(
            src_ref=view(part),
            dst_ref=view(part),
            send_sem=xsend.at[i, q],
            recv_sem=xrecv.at[i, part],
            device_id=(me, lax.rem(tp + q, group)),
            device_id_type=MESH,
        )

    def swap_start(view, i):
        for q in range(1, group):
            swap(view, i, tp, q).start()

    def swap_recv(view, i):
        for q in range(1, group):
            swap(view, i, lax.rem(tp + q, group), q).wait_recv()

    def swap_sent(view, i):
        for q in range(1, group):
            swap(view, i, tp, q).wait_send()

    def hidden_view(s):
        return lambda part: hbuf.at[part, s]

    def shared_view(part):
        return shbuf.at[part]

    def squares_view(part):
        return sq.at[part]

    def scatter(s, ch):
        @pl.loop(1, mates)
        def _(k):
            dispatch(s, ch, turn(k), spot).start()

        stay(s, ch).start()

    def pass_on(s, ch):
        stay(s, ch).wait()
        for q in range(1, group):
            forward(tp, s, ch, spot, q).start()

        @pl.loop(1, mates)
        def _(k):
            source = turn(mates - k)
            dispatch(s, ch, source, source).wait_recv()
            for q in range(1, group):
                forward(tp, s, ch, source, q).start()

    def passed(s, part, q):
        for ch in range(chunks):

            @pl.loop(0, mates)
            def _(k):
                forward(part, s, ch, turn(mates - k), q).wait_recv()

    pl.semaphore_wait(barrier, mates - 1 + 1 + group - 1)

    cross_info().start()
    for ch in range(chunks):
        cross(ch).start()
    for ch in range(chunks):
        scatter(OWN, ch)

    for q in range(1, group):
        normalize(lax.rem(tp + q, group))
    loads[0].wait()
    loads[1].wait()
    wide_k = min(512, half)
    acc_g[0, :rows] = jnp.zeros((rows, vsg.shape[0]), F32)
    acc_u[0, :rows] = jnp.zeros((rows, vsu.shape[0]), F32)
    for h in range(group):

        @pl.loop(0, half // wide_k)
        def _(c):
            cols = pl.ds(pl.multiple_of(c * wide_k, wide_k), wide_k)
            wide = pl.ds(pl.multiple_of(h * half + c * wide_k, wide_k), wide_k)
            xs = nrm[h, :, cols]
            acc_g[0, :rows] += dot_nt(xs, vsg[:, wide])
            acc_u[0, :rows] += dot_nt(xs, vsu[:, wide])

    shbuf[tp] = silu_mul(acc_g[0, :rows], acc_u[0, :rows]).astype(BF16)
    swap_start(shared_view, SHARED)

    cross_info().wait_recv()
    far_weight = far_info[:, :rows]
    far_picker = pickers(far_weight)
    for ch in range(chunks):
        cross(ch).wait_recv()
        pick(far_picker, lambda at: far_x[:, at : at + kc], FAR, ch)
        scatter(FAR, ch)

    row_piece = lax.broadcasted_iota(jnp.int32, (slots, kc), 0) % 8 // rest if rest else None

    def project(s, part, first):
        for ch in range(chunks):
            pieces = [recv[part, s, ch, :, i * span : (i + 1) * span] for i in range(fulls)]
            if rest:
                last = recv[part, s, ch, :, fulls * span :]
                pieces.append(
                    jnp.concatenate(
                        [jnp.where(row_piece == c, last, jnp.zeros_like(last)) for c in range(folds)],
                        axis=1,
                    )
                )
            xs = jnp.concatenate(pieces, axis=0)
            wide = pl.ds(pl.multiple_of(part * half + ch * span, span), span)
            g = dot_nt(xs, vg[:, wide])
            u = dot_nt(xs, vu[:, wide])
            if first and ch == 0:
                acc_g[s] = g
                acc_u[s] = u
            else:
                acc_g[s] += g
                acc_u[s] += u

    def activate(s):
        for i in range(blocks):
            at = slice(i * slots, (i + 1) * slots)
            g, u = acc_g[s, at], acc_u[s, at]
            if i == fulls:
                g = g.reshape(mates, 8, -1)
                u = u.reshape(mates, 8, -1)
                shift = rest
                while shift < 8:
                    g = g + pltpu.roll(g, shift, 1)
                    u = u + pltpu.roll(u, shift, 1)
                    shift *= 2
                g = g.reshape(slots, -1)
                u = u.reshape(slots, -1)
            hbuf[tp, s, at] = silu_mul(g, u).astype(BF16)
        swap_start(hidden_view(s), HIDDEN + s)

    def down(hidden, weights, at):
        depth = weights.shape[0] // group
        return sum(
            dot_nn(hidden(p), weights[p * depth : (p + 1) * depth, at : at + kc])
            for p in range(group)
        )

    def respond(s):
        for ch in range(chunks):
            for c in range(span // kc):
                made = down(lambda p: hbuf[p, s], vd, ch * span + c * kc)
                for i in range(fulls):
                    outb[s, ch, :, i * span + c * kc : i * span + (c + 1) * kc] = made[
                        i * slots : (i + 1) * slots
                    ].astype(BF16)
                if rest:
                    fresh = made[fulls * slots :]
                    last = fresh if c == 0 else jnp.where(row_piece == c, fresh, last)
            if rest:
                outb[s, ch, :, fulls * span :] = last.astype(BF16)

            @pl.loop(1, mates)
            def _(k):
                give_back(s, ch, turn(k), spot).start()

            stay_back(s, ch).start()

    for ch in range(chunks):
        pass_on(OWN, ch)
    loads[2].wait()
    loads[3].wait()
    project(OWN, tp, True)
    for q in range(1, group):
        part = lax.rem(tp + q, group)
        passed(OWN, part, q)
        project(OWN, part, False)
    activate(OWN)

    for ch in range(chunks):
        pass_on(FAR, ch)
    project(FAR, tp, True)
    loads[4].wait()
    swap_recv(hidden_view(OWN), HIDDEN + OWN)
    respond(OWN)
    for q in range(1, group):
        part = lax.rem(tp + q, group)
        passed(FAR, part, q)
        project(FAR, part, False)
    activate(FAR)
    swap_recv(hidden_view(FAR), HIDDEN + FAR)
    respond(FAR)

    loads[5].wait()
    swap_recv(shared_view, SHARED)
    for at in range(0, half, kc):
        comb[:, at : at + kc] = down(lambda p: shbuf[p], vsd, at)

    def came_back(s, ch):
        stay_back(s, ch).wait()

        @pl.loop(1, mates)
        def _(k):
            source = turn(mates - k)
            give_back(s, ch, source, source).wait_recv()

    def mix(mixer, s, ch, c):
        listed, coarse, fine = mixer
        backs, tops, lows = [], [], []
        for i, (taken, piece) in enumerate(listed):
            if piece is None:
                backs.append(ret[s, ch, :, i * span + c * kc : i * span + (c + 1) * kc])
            else:
                backs.append(ret[s, ch, :, fulls * span :])
                taken = taken & (piece == c)
            tops.append(jnp.where(taken, coarse, 0.0))
            lows.append(jnp.where(taken, fine, 0.0))
        both = jnp.concatenate(
            [jnp.concatenate(tops, axis=1), jnp.concatenate(lows, axis=1)], axis=0
        )
        mixed = dot_nn(both.astype(BF16), jnp.concatenate(backs, axis=0))
        return mixed[:rows] + mixed[rows:]

    far_mixer = mixers(far_weight)
    for ch in range(chunks):
        came_back(FAR, ch)
        for c in range(span // kc):
            at = ch * span + c * kc
            psend[:, at : at + kc] = mix(far_mixer, FAR, ch, c).astype(BF16)
        cross_back(ch).start()

    own_mixer = mixers(own_weight)
    for ch in range(chunks):
        came_back(OWN, ch)
        for c in range(span // kc):
            at = ch * span + c * kc
            comb[:, at : at + kc] += mix(own_mixer, OWN, ch, c)

    total = jnp.zeros((rows, 1), F32)
    for ch in range(chunks):
        cross_back(ch).wait_recv()
        for c in range(span // kc):
            at = ch * span + c * kc
            part = comb[:, at : at + kc] + precv[:, at : at + kc].astype(F32)
            comb[:, at : at + kc] = part
            total = total + jnp.sum(part * part, axis=1, keepdims=True)
    sq[tp] = jnp.broadcast_to(total, sq.shape[1:])
    swap_start(squares_view, SQUARES)

    cross_info().wait_send()
    for ch in range(chunks):
        cross(ch).wait_send()
        cross_back(ch).wait_send()
        for s in (OWN, FAR):

            @pl.loop(1, mates)
            def _(k):
                dispatch(s, ch, turn(k), spot).wait_send()
                give_back(s, ch, turn(k), spot).wait_send()

            @pl.loop(0, mates)
            def _(k):
                for q in range(1, group):
                    forward(tp, s, ch, k, q).wait_send()

    swap_sent(shared_view, SHARED)
    for s in (OWN, FAR):
        swap_sent(hidden_view(s), HIDDEN + s)
    smalls[4].wait()
    swap_recv(squares_view, SQUARES)
    norm = lax.rsqrt(sum(sq[p] for p in range(group))[:, :1] / width + EPS)
    o[...] = (comb[...] * norm * outg[...]).astype(BF16)
    swap_sent(squares_view, SQUARES)


def on_device(experts, tokens, in_gain, routes, gates, eg, eu, ed, sg, su, sd, out_gain):
    rows, width = tokens.shape
    topk = routes.shape[1]
    group = lax.axis_size("tp")
    half = width // group
    cap = min(rows, (rows * topk + experts - 1) // experts + 1)
    fulls, rest = cap // 8, cap % 8
    while rest & (rest - 1):
        rest += 1
    if rest and half * rest // 8 % 128:
        rest = 8
    if rest == 8:
        fulls, rest = fulls + 1, 0
    chunks = 1 if half // 2 * (rest or 8) // 8 % 128 else 2
    mates = experts // 2
    slots = mates * 8
    blocks = fulls + (1 if rest else 0)
    span = half // chunks
    packed = fulls * span + span * rest // 8
    hid, shid = eg.shape[1], sg.shape[0]
    deep = max(blocks * slots, rows)
    vmem = pl.BlockSpec(memory_space=pltpu.VMEM)
    hbm = pl.BlockSpec(memory_space=pl.ANY)
    dma = pltpu.SemaphoreType.DMA
    sets = (2, chunks, slots, packed)
    assert deep == blocks * slots and hid == shid and mates * 2 == experts
    return pl.pallas_call(
        functools.partial(kernel, experts, fulls, rest, chunks),
        out_shape=jax.ShapeDtypeStruct((rows, half), BF16),
        in_specs=[hbm] * 11,
        out_specs=vmem,
        scratch_shapes=[
            pltpu.VMEM((rows, width), BF16),
            pltpu.VMEM((1, width), F32),
            pltpu.VMEM((topk, rows), jnp.int32),
            pltpu.VMEM((topk, rows), F32),
            pltpu.VMEM((1, half), F32),
            pltpu.VMEM(eg.shape[1:], BF16),
            pltpu.VMEM(eu.shape[1:], BF16),
            pltpu.VMEM(ed.shape[1:], BF16),
            pltpu.VMEM(sg.shape, BF16),
            pltpu.VMEM(su.shape, BF16),
            pltpu.VMEM(sd.shape, BF16),
            pltpu.VMEM((group, rows, half), BF16),
            pltpu.VMEM((rows, half), BF16),
            pltpu.VMEM((mates, 128), F32),
            pltpu.VMEM((mates, 128), F32),
            pltpu.VMEM(sets, BF16),
            pltpu.VMEM((group,) + sets, BF16),
            pltpu.VMEM((2, deep, hid), F32),
            pltpu.VMEM((2, deep, hid), F32),
            pltpu.VMEM((group, 2, blocks * slots, hid), BF16),
            pltpu.VMEM((group, rows, shid), BF16),
            pltpu.VMEM(sets, BF16),
            pltpu.VMEM(sets, BF16),
            pltpu.VMEM((rows, half), BF16),
            pltpu.VMEM((rows, half), BF16),
            pltpu.VMEM((rows, half), F32),
            pltpu.VMEM((group, rows, 128), F32),
            dma((5,)),
            dma((6,)),
            dma((2, 2, chunks)),
            dma((chunks + 1,)),
            dma((chunks + 1,)),
            dma((2, chunks, mates)),
            dma((2, chunks, mates)),
            dma((group, 2, chunks, mates)),
            dma((group, 2, chunks, mates)),
            dma((2, chunks, mates)),
            dma((2, chunks, mates)),
            dma((chunks,)),
            dma((chunks,)),
            dma((4, group)),
            dma((4, group)),
        ],
        compiler_params=pltpu.CompilerParams(
            collective_id=0, has_side_effects=True, vmem_limit_bytes=60 * 1024 * 1024
        ),
    )(
        tokens, in_gain.reshape(1, width), routes.T, gates.T, eg, eu, ed, sg, su, sd,
        out_gain.reshape(1, half),
    )


def solution(mesh):
    in_specs = (
        P("ep", None),
        P(),
        P("ep", None),
        P("ep", None),
        P("ep", "tp", None),
        P("ep", "tp", None),
        P("ep", None, "tp"),
        P("tp", None),
        P("tp", None),
        P(None, "tp"),
        P("tp"),
    )
    return jax.shard_map(
        functools.partial(on_device, mesh.shape["ep"]),
        mesh=mesh,
        in_specs=in_specs,
        out_specs=P("ep", "tp"),
        check_vma=False,
    )
```
